32 devices in a mesh: rep: 2 (over x), fs: 8 (over z, y), tp: 2 (over core).
Axes of the slice: x: 2, y: 2, z: 4, core: 2. Of those that a mesh axis runs over, the one named last changes fastest.
Arguments:
- hidden_in: bfloat16 [12288, 2048], P(('rep', 'fs', 'tp')), may hold values from -6 to 6
- norm_gain: float32 [2048], replicated, may hold values from 0.1 to 1.9
- up_weight: float32 [2048, 8192], P('fs', 'tp'), may hold values from -0.125 to 0.125
- up_scale: float32 [8192], P('tp'), may hold values from 0.5 to 2
- down_weight: float32 [8192, 2048], P('tp', 'fs'), may hold values from -0.0625 to 0.0625
- down_scale: float32 [2048], replicated, may hold values from 0.5 to 2
Outputs:
- layer_out: bfloat16 [12288, 2048], P(('rep', 'fs', 'tp'))
The draws below stay inside these ranges and needn't reach their ends.
All inputs are finite; a program needn't handle non-finite values.
Results may differ from the reference program's by a relative error of at most 0.0085.
Values may be sent and summed in bfloat16 or wider, within the bound.
A program may use at most 128 MiB of HBM per device.

```python
import math
import jax
import jax.numpy as jnp
from jax import lax

D = 2048
FF = 8192
TOKENS = 12288
N_TP = 2


def shard_levels(rng, shape, split, smallest, high):
    def one(dim, parts):
        draws = jax.random.uniform(jax.random.fold_in(jax.random.fold_in(rng, 6), dim), (parts,), jnp.float32, smallest / len(split), high / len(split))
        return jnp.repeat(jnp.exp(draws), shape[dim] // parts).reshape((-1,) + (1,) * (len(shape) - dim - 1))

    level = one(*split[0])
    for cut in split[1:]:
        level = level * one(*cut)
    return level


def normal_values(stream_key, shape, deviation, most, pieces=(), kind=jnp.bfloat16):
    level = shard_levels(stream_key, shape, pieces, -0.22, 0.18) if pieces else 1.0
    values = jax.random.normal(stream_key, shape, jnp.float32) * deviation * level
    return jnp.minimum(jnp.maximum(values, -most), most).astype(kind)


def setup_inputs(seed: int = 0) -> dict:
    seeds = jax.random.split(jax.random.key(seed), 7)
    return {
        "hidden_in": normal_values(seeds[0], (TOKENS, D), 1.0, 6.0, ((0, 32),)),
        "norm_gain": jnp.clip(1.0 + 0.18 * jax.random.normal(seeds[1], (D,), jnp.float32), 0.1, 1.9),
        "up_weight": normal_values(seeds[2], (D, FF), D ** -0.5, 0.125, ((0, 8), (1, 2)), jnp.float32),
        "up_scale": jnp.clip(jnp.exp(math.log(2.0) - 1.3862944 * jax.random.uniform(seeds[3], (FF,), jnp.float32) ** shard_levels(seeds[3], (FF,), ((0, 2),), -0.2, 0.2)), 0.5, 2.0),
        "down_weight": normal_values(seeds[4], (FF, D), FF ** -0.5, 0.0625, ((0, 2), (1, 8)), jnp.float32),
        "down_scale": jnp.clip(jnp.exp(jax.random.uniform(seeds[5], (D,), jnp.float32, math.log(0.5), math.log(2.0))), 0.5, 2.0),
    }


def reference(hidden_in, norm_gain, up_weight, up_scale, down_weight, down_scale):
    up_low = up_weight.astype(jnp.bfloat16)
    down_low = down_weight.astype(jnp.bfloat16)
    block = math.gcd(2048, TOKENS)
    width = FF // N_TP

    def one_block(start):
        rows = lax.dynamic_slice_in_dim(hidden_in, start, block, 0).astype(jnp.float32)
        normed = (rows * lax.rsqrt(lax.optimization_barrier(jnp.mean(rows * rows, axis=1, keepdims=True)) + 1e-06) * norm_gain).astype(jnp.bfloat16)
        pre = jnp.dot(normed, up_low, preferred_element_type=jnp.float32) * up_scale
        act = jnp.square(jnp.maximum(pre, 0.0)).astype(jnp.bfloat16)
        total = jnp.zeros((block, D), jnp.float32)
        for index in range(N_TP):
            part = jnp.dot(act[:, index * width:(index + 1) * width], down_low[index * width:(index + 1) * width], preferred_element_type=jnp.float32).astype(jnp.bfloat16)
            part = lax.optimization_barrier(part)
            total = total + part.astype(jnp.float32)
        return (total * down_scale).astype(jnp.bfloat16)
    starts = jnp.arange(0, TOKENS, block, dtype=jnp.int32)
    outs = lax.map(one_block, starts)
    return outs.reshape(TOKENS, D)
```

```python
import functools

import jax
import jax.numpy as jnp
from jax import lax
from jax.experimental import pallas as pl
from jax.experimental.pallas import tpu as pltpu
from jax.sharding import Mesh, PartitionSpec as P

MESH = pl.DeviceIdType.MESH
LOW = jnp.bfloat16


def kernel(
    n, hidden, gain, up_f32, up_scale, dn_f32, dn_scale, out,
    hid, up_st, dn_st, up_peer, dn_peer,
    tok, up_w, dn_w, act, psend, precv, csum, ra1, rb1, ra2, rb2,
    up_rs, up_sr, up_sl, dn_rs, dn_sr, dn_sl, ss, rs, ls,
):
    x, z, y, c = (lax.axis_index(a) for a in ("rep", "fz", "fy", "tp"))
    ox, oy, oc = 1 - x, 1 - y, 1 - c
    to_x, to_y, to_c = {"rep": ox}, {"fy": oy}, {"tp": oc}
    to_right = {"fz": jnp.minimum(z + 1, n - 1)}
    to_left = {"fz": jnp.maximum(z - 1, 0)}
    has_right, has_left = z < n - 1, z > 0
    tiles, kr, tile = up_peer.shape
    nsub, width, pc = dn_peer.shape
    rows, depth = hid.shape
    cols = nsub * pc
    steps = n * nsub
    top = max(rows // 48, 1) * 16

    def quarter(yy):
        return pl.ds(pl.multiple_of((x * 2 + yy) * width, width), width)

    loads = [
        pltpu.make_async_copy(up_f32.at[:, quarter(y)], up_st.at[0], ls.at[0]),
        pltpu.make_async_copy(up_f32.at[:, quarter(oy)], up_st.at[1], ls.at[1]),
        pltpu.make_async_copy(hidden, hid, ls.at[2]),
        pltpu.make_async_copy(dn_f32.at[quarter(y)], dn_st.at[0], ls.at[3]),
        pltpu.make_async_copy(dn_f32.at[quarter(oy)], dn_st.at[1], ls.at[4]),
    ]
    barrier = pltpu.get_barrier_semaphore()
    for other in (to_x, to_y, to_c):
        pl.semaphore_signal(barrier, inc=1, device_id=other, device_id_type=MESH)

    @pl.when(has_right)
    def _():
        pl.semaphore_signal(barrier, inc=1, device_id=to_right, device_id_type=MESH)

    @pl.when(has_left)
    def _():
        pl.semaphore_signal(barrier, inc=1, device_id=to_left, device_id_type=MESH)

    for copy in loads:
        copy.start()
    here = pl.ds(pl.multiple_of((z * 2 + y) * kr, kr), kr)
    loads[0].wait()
    for j in range(tiles):
        up_w[j, here] = up_st[0, :, j * tile:(j + 1) * tile].astype(LOW)
    loads[1].wait()
    for j in range(tiles):
        up_peer[j] = up_st[1, :, j * tile:(j + 1) * tile].astype(LOW)
    pl.semaphore_wait(barrier, 3 + jnp.minimum(z, 1) + jnp.minimum(n - 1 - z, 1))

    count = [0]
    sent = []

    def remote(src, dst, send_sem, recv_sem, other):
        return pltpu.make_async_remote_copy(
            src_ref=src, dst_ref=dst, send_sem=send_sem, recv_sem=recv_sem,
            device_id=other, device_id_type=MESH,
        )

    def send(src, dst, other):
        i = count[0]
        count[0] += 1
        copy = remote(src, dst, ss.at[i], rs.at[i], other)
        copy.start()
        sent.append(copy)
        return copy

    def up_piece(j, o, yy, right):
        shard = o * 2 + yy
        ref = up_w.at[j, pl.ds(pl.multiple_of(shard * kr, kr), kr)]
        sems = up_sr if right else up_sl
        return remote(ref, ref, sems.at[j, shard], up_rs.at[j, shard], to_right if right else to_left)

    def dn_piece(u, o, yy, right):
        ref = dn_w.at[o, u, yy]
        sems = dn_sr if right else dn_sl
        return remote(
            ref, ref, sems.at[u, o * 2 + yy], dn_rs.at[u, o * 2 + yy], to_right if right else to_left
        )

    def own_pieces(piece, i, yy):
        @pl.when(has_right)
        def _():
            piece(i, z, yy, True).start()

        @pl.when(has_left)
        def _():
            piece(i, z, yy, False).start()

    def ends(t):
        return jnp.maximum(z - t, 0), jnp.minimum(z + t, n - 1)

    def pass_on(piece, i, t):
        before, after = ends(t)

        @pl.when(z - t >= 0)
        def _():
            for yy in (y, oy):
                piece(i, before, yy, True).wait_recv()

                @pl.when(has_right)
                def _():
                    piece(i, before, yy, True).start()

        @pl.when(z + t < n)
        def _():
            for yy in (y, oy):
                piece(i, after, yy, False).wait_recv()

                @pl.when(has_left)
                def _():
                    piece(i, after, yy, False).start()

    def all_sent(piece, i):
        @pl.loop(0, n)
        def _(t):
            before, after = ends(t)
            for yy in (y, oy):
                @pl.when(jnp.logical_and(z - t >= 0, has_right))
                def _():
                    piece(i, before, yy, True).wait_send()

                @pl.when(jnp.logical_and(z + t < n, has_left))
                def _():
                    piece(i, after, yy, False).wait_send()

    own_pieces(up_piece, 0, y)
    y_up = [send(up_peer.at[j], up_w.at[j, here], to_y) for j in range(tiles)]

    loads[2].wait()
    block = min(64, rows)

    @pl.loop(0, rows // block)
    def _(i):
        at = pl.ds(pl.multiple_of(i * block, block), block)
        wide = hid[at].astype(jnp.float32)
        scale = lax.rsqrt(jnp.mean(wide * wide, axis=1, keepdims=True) + 1e-06)
        tok[x, y, c, at] = (wide * scale * gain[...]).astype(LOW)

    loads[3].wait()
    for u in range(nsub):
        dn_w[z, u, y] = dn_st[0, :, u * pc:(u + 1) * pc].astype(LOW)
    loads[4].wait()
    for u in range(nsub):
        dn_peer[u] = dn_st[1, :, u * pc:(u + 1) * pc].astype(LOW)

    def token_part(xx, yy, first):
        return tok.at[xx, yy, c, pl.ds(0, top) if first else pl.ds(top, rows - top)]

    tx = [send(token_part(x, y, f), token_part(x, y, f), to_x) for f in (True, False)]
    ty = [send(token_part(x, y, f), token_part(x, y, f), to_y) for f in (False, True)]
    tc = send(tok.at[x, y, c], tok.at[x, y, c], to_c)

    def own_up(j):
        own_pieces(up_piece, j, y)

    def peer_up(j):
        y_up[j].wait_recv()
        own_pieces(up_piece, j, oy)

    def up_unit(gx, gy, j):
        at = pl.ds(pl.multiple_of(j * tile, tile), tile)
        sc_at = pl.ds(pl.multiple_of((x * 2 + y) * width + j * tile, tile), tile)
        pre = jnp.dot(
            tok[gx, gy].reshape(2 * rows, depth), up_w[j], preferred_element_type=jnp.float32
        )
        value = jnp.square(jnp.maximum(pre * up_scale[:, sc_at], 0.0)).astype(LOW)
        act[0, gx, gy, :, at] = value[:rows]
        act[1, gx, gy, :, at] = value[rows:]

    peer_up(0)
    if tiles > 1:
        own_up(1)
        peer_up(1)

    late = {}
    for j in range(tiles):
        last = j == tiles - 1
        if 2 <= j + 1 < tiles:
            own_up(j + 1)
            peer_up(j + 1)
        if last:
            own_pieces(dn_piece, 0, y)
        for t in range(1, n):
            pass_on(up_piece, j, t)
            if j == 0 and t == n - 1:
                tx[0].wait_recv()
                late["diag_y"] = send(token_part(ox, y, True), token_part(ox, y, True), to_y)
                late["y_dn"] = [send(dn_peer.at[u], dn_w.at[z, u, y], to_y) for u in range(nsub)]
            if j == tiles // 2 - 1 and t == n - 1:
                ty[0].wait_recv()
                late["diag_x"] = send(token_part(x, oy, False), token_part(x, oy, False), to_x)
                tx[1].wait_recv()
                cx = send(tok.at[ox, y, c], tok.at[ox, y, c], to_c)
            if j == tiles - 2:
                if t == max(1, n // 3):
                    tc.wait_recv()
                    cx.wait_recv()

                    @pl.loop(0, 2 * (tiles - 2))
                    def _(i):
                        g = i % 2
                        up_unit(x + g * (ox - x), y, i // 2)
                if t == max(1, (2 * n) // 3):
                    ty[1].wait_recv()
                    cy = send(tok.at[x, oy, c], tok.at[x, oy, c], to_c)
            if last:
                if t == 1:
                    cy.wait_recv()

                    @pl.loop(0, tiles - 1)
                    def _(i):
                        up_unit(x, oy, i)
                if t == max(1, n // 3):
                    late["diag_y"].wait_recv()
                    late["diag_x"].wait_recv()
                    cd = send(tok.at[ox, oy, c], tok.at[ox, oy, c], to_c)

                    @pl.loop(0, 2)
                    def _(g):
                        up_unit(x + g * (ox - x), y, tiles - 2)
                if t == max(1, (2 * n) // 3):
                    cd.wait_recv()

                    @pl.loop(0, tiles - 1)
                    def _(i):
                        up_unit(ox, oy, i)
    late["y_dn"][0].wait_recv()
    own_pieces(dn_piece, 0, oy)
    for u in range(1, nsub):
        own_pieces(dn_piece, u, y)
        late["y_dn"][u].wait_recv()
        own_pieces(dn_piece, u, oy)

    @pl.loop(0, 4)
    def _(i):
        up_unit(i // 2, i % 2, tiles - 1)

    side = jnp.minimum(z, n - 1 - z)
    far = jnp.where(z <= n - 1 - z, 1, -1)

    def owner(s):
        p = s // nsub
        near = z + (-1 if p % 2 else 1) * ((p + 1) // 2)
        return jnp.where(p <= 2 * side, near, z + far * (p - side))

    def each_part(s, cc, emit):
        o, u = owner(s), s % nsub

        @pl.loop(0, 2)
        def _(xx):
            left = act[cc, xx].reshape(2 * rows, width)
            if pc % 128 == 0:
                right = jnp.concatenate([dn_w[o, u, 0], dn_w[o, u, 1]], axis=1)
                both = jnp.dot(left, right, preferred_element_type=jnp.float32)
                halves = both[:, :pc], both[:, pc:]
            else:
                halves = [
                    jnp.dot(left, dn_w[o, u, yy], preferred_element_type=jnp.float32)
                    for yy in range(2)
                ]
            for yy in range(2):
                at = slice(yy * rows, (yy + 1) * rows)
                emit(0, xx, yy, halves[0][at].astype(LOW))
                emit(1, yy, xx, halves[1][at].astype(LOW))

    given, first, second = {}, {}, {}

    def for_partner(s):
        p = s % 2
        if s >= 2:
            given[s - 2].wait_send()

        def emit(h, f, g, part):
            psend[p, h, f, g] = part

        each_part(s, oc, emit)
        given[s] = send(psend.at[p], precv.at[s], to_c)

    def for_own(s):
        p = s % 2

        def emit(h, f, g, part):
            csum[p, h, f, g] = part

        each_part(s, c, emit)
        given[s].wait_recv()
        total = csum[p].astype(jnp.float32) + precv[s].astype(jnp.float32)
        csum[p] = total.astype(LOW)
        first[s] = (
            send(csum.at[p, 0, ox], ra1.at[s], to_x),
            send(csum.at[p, 1, oy], rb1.at[s], to_y),
        )

    def second_stage(s):
        p = s % 2
        pair = []
        for h, f, g, got, dst, other in (
            (0, x, oy, ra1, ra2, to_y), (1, y, ox, rb1, rb2, to_x)
        ):
            first[s][h].wait_recv()
            total = csum[p, h, f, g].astype(jnp.float32) + got[s, g].astype(jnp.float32)
            csum[p, h, f, g] = total.astype(LOW)
            pair.append(send(csum.at[p, h, f, g], dst.at[s], other))
        second[s] = pair

    def finish(s):
        p = s % 2
        o, u = owner(s), s % nsub
        for h, f, g, one, two in ((0, x, y, ra1, ra2), (1, y, x, rb1, rb2)):
            second[s][h].wait_recv()
            total = csum[p, h, f, g].astype(jnp.float32) + one[s, g].astype(jnp.float32)
            total = total + two[s].astype(jnp.float32)
            slot = (o * 2 + h) * nsub + u
            if pc % 128 == 0:
                at = pl.ds(pl.multiple_of(slot * pc, pc), pc)
                out[:, at] = (total * dn_scale[:, at]).astype(out.dtype)
            else:
                out[slot] = (total * dn_scale[slot]).astype(out.dtype)
        for copy in (*first[s], *second[s]):
            copy.wait_send()

    for s in range(steps):
        for_partner(s)
        if s >= 2:
            finish(s - 2)
        for_own(s)
        second_stage(s)
        e = s - nsub + 1
        if 0 <= e < (n - 1) * nsub:
            pass_on(dn_piece, e % nsub, e // nsub + 1)
    finish(steps - 2)
    finish(steps - 1)
    for j in range(tiles):
        all_sent(up_piece, j)
    for u in range(nsub):
        all_sent(dn_piece, u)
    for copy in (
        *y_up, *tx, *ty, tc, late["diag_y"], *late["y_dn"], late["diag_x"], cx, cy, cd,
        given[steps - 2], given[steps - 1],
    ):
        copy.wait_send()


def body(hidden_in, norm_gain, up_weight, up_scale, down_weight, down_scale):
    n = lax.axis_size("fz")
    rows, depth = hidden_in.shape
    kr, cols = up_weight.shape[0], down_weight.shape[1]
    width = up_weight.shape[1] // 4
    tile = min(256, width)
    tiles = width // tile
    pc = min(128, cols)
    nsub = cols // pc
    steps = n * nsub
    flat = pc % 128 == 0
    sends = tiles + 10 + nsub + 5 * steps
    vmem = pl.BlockSpec(memory_space=pltpu.VMEM)
    hbm = pl.BlockSpec(memory_space=pl.ANY)
    dma = pltpu.SemaphoreType.DMA
    made = pl.pallas_call(
        functools.partial(kernel, n),
        out_shape=jax.ShapeDtypeStruct((rows, depth) if flat else (2 * steps, rows, pc), LOW),
        in_specs=[hbm, vmem, hbm, vmem, hbm, vmem],
        out_specs=vmem,
        scratch_shapes=[
            pltpu.VMEM((rows, depth), LOW),
            pltpu.VMEM((2, kr, width), jnp.float32),
            pltpu.VMEM((2, width, cols), jnp.float32),
            pltpu.VMEM((tiles, kr, tile), LOW),
            pltpu.VMEM((nsub, width, pc), LOW),
            pltpu.VMEM((2, 2, 2, rows, depth), LOW),
            pltpu.VMEM((tiles, depth, tile), LOW),
            pltpu.VMEM((n, nsub, 2, width, pc), LOW),
            pltpu.VMEM((2, 2, 2, rows, width), LOW),
            pltpu.VMEM((2, 2, 2, 2, rows, pc), LOW),
            pltpu.VMEM((steps, 2, 2, 2, rows, pc), LOW),
            pltpu.VMEM((2, 2, 2, 2, rows, pc), LOW),
            pltpu.VMEM((steps, 2, rows, pc), LOW),
            pltpu.VMEM((steps, 2, rows, pc), LOW),
            pltpu.VMEM((steps, rows, pc), LOW),
            pltpu.VMEM((steps, rows, pc), LOW),
            dma((tiles, 2 * n)), dma((tiles, 2 * n)), dma((tiles, 2 * n)),
            dma((nsub, 2 * n)), dma((nsub, 2 * n)), dma((nsub, 2 * n)),
            dma((sends,)), dma((sends,)), dma((5,)),
        ],
        compiler_params=pltpu.CompilerParams(
            collective_id=0, has_side_effects=True, vmem_limit_bytes=64000 * 1024
        ),
    )(
        hidden_in,
        norm_gain.reshape(1, depth),
        up_weight,
        up_scale.reshape(1, 4 * width),
        down_weight,
        down_scale.reshape((1, depth) if flat else (2 * steps, 1, pc)),
    )
    return made if flat else made.transpose(1, 0, 2).reshape(rows, depth)


def solution(mesh):
    n_rep, n_fs, n_tp = (mesh.shape[a] for a in ("rep", "fs", "tp"))
    split = Mesh(mesh.devices.reshape(n_rep, n_fs // 2, 2, n_tp), ("rep", "fz", "fy", "tp"))
    fs = ("fz", "fy")
    tokens = P(("rep", *fs, "tp"), None)
    placed = (tokens, P(), P(fs, "tp"), P("tp"), P("tp", fs), P())
    return jax.shard_map(body, mesh=split, in_specs=placed, out_specs=tokens, check_vma=False)
```

```python
import functools

import jax
import jax.numpy as jnp
from jax import lax
from jax.experimental import pallas as pl
from jax.experimental.pallas import tpu as pltpu
from jax.sharding import Mesh, PartitionSpec as P

MESH = pl.DeviceIdType.MESH
LOW = jnp.bfloat16


def kernel(
    n, hidden, gain, up_f32, up_scale, dn_f32, dn_scale, out,
    hid, up_st, dn_st, up_peer, dn_peer,
    tok, up_w, dn_w, act, psend, precv, csum, ra1, rb1, ra2, rb2,
    up_rs, up_sr, up_sl, dn_rs, dn_sr, dn_sl, ss, rs, ls,
):
    x, z, y, c = (lax.axis_index(a) for a in ("rep", "fz", "fy", "tp"))
    ox, oy, oc = 1 - x, 1 - y, 1 - c
    to_x, to_y, to_c = {"rep": ox}, {"fy": oy}, {"tp": oc}
    to_right = {"fz": jnp.minimum(z + 1, n - 1)}
    to_left = {"fz": jnp.maximum(z - 1, 0)}
    has_right, has_left = z < n - 1, z > 0
    tiles, kr, tile = up_peer.shape
    nsub, width, pc = dn_peer.shape
    rows, depth = hid.shape
    cols = nsub * pc
    steps = n * nsub
    top = max(rows // 48, 1) * 16

    def quarter(yy):
        return pl.ds(pl.multiple_of((x * 2 + yy) * width, width), width)

    loads = [
        pltpu.make_async_copy(up_f32.at[:, quarter(y)], up_st.at[0], ls.at[0]),
        pltpu.make_async_copy(up_f32.at[:, quarter(oy)], up_st.at[1], ls.at[1]),
        pltpu.make_async_copy(hidden, hid, ls.at[2]),
        pltpu.make_async_copy(dn_f32.at[quarter(y)], dn_st.at[0], ls.at[3]),
        pltpu.make_async_copy(dn_f32.at[quarter(oy)], dn_st.at[1], ls.at[4]),
    ]
    barrier = pltpu.get_barrier_semaphore()
    for other in (to_x, to_y, to_c):
        pl.semaphore_signal(barrier, inc=1, device_id=other, device_id_type=MESH)

    @pl.when(has_right)
    def _():
        pl.semaphore_signal(barrier, inc=1, device_id=to_right, device_id_type=MESH)

    @pl.when(has_left)
    def _():
        pl.semaphore_signal(barrier, inc=1, device_id=to_left, device_id_type=MESH)

    for copy in loads:
        copy.start()
    here = pl.ds(pl.multiple_of((z * 2 + y) * kr, kr), kr)
    loads[0].wait()
    for j in range(tiles):
        up_w[j, here] = up_st[0, :, j * tile:(j + 1) * tile].astype(LOW)
    loads[1].wait()
    for j in range(tiles):
        up_peer[j] = up_st[1, :, j * tile:(j + 1) * tile].astype(LOW)
    pl.semaphore_wait(barrier, 3 + jnp.minimum(z, 1) + jnp.minimum(n - 1 - z, 1))

    count = [0]
    sent = []

    def remote(src, dst, send_sem, recv_sem, other):
        return pltpu.make_async_remote_copy(
            src_ref=src, dst_ref=dst, send_sem=send_sem, recv_sem=recv_sem,
            device_id=other, device_id_type=MESH,
        )

    def send(src, dst, other):
        i = count[0]
        count[0] += 1
        copy = remote(src, dst, ss.at[i], rs.at[i], other)
        copy.start()
        sent.append(copy)
        return copy

    def up_piece(j, o, yy, right):
        shard = o * 2 + yy
        ref = up_w.at[j, pl.ds(pl.multiple_of(shard * kr, kr), kr)]
        sems = up_sr if right else up_sl
        return remote(ref, ref, sems.at[j, shard], up_rs.at[j, shard], to_right if right else to_left)

    def dn_piece(u, o, yy, right):
        ref = dn_w.at[o, u, yy]
        sems = dn_sr if right else dn_sl
        return remote(
            ref, ref, sems.at[u, o * 2 + yy], dn_rs.at[u, o * 2 + yy], to_right if right else to_left
        )

    def own_pieces(piece, i, yy):
        @pl.when(has_right)
        def _():
            piece(i, z, yy, True).start()

        @pl.when(has_left)
        def _():
            piece(i, z, yy, False).start()

    def ends(t):
        return jnp.maximum(z - t, 0), jnp.minimum(z + t, n - 1)

    def pass_on(piece, i, t):
        before, after = ends(t)

        @pl.when(z - t >= 0)
        def _():
            for yy in (y, oy):
                piece(i, before, yy, True).wait_recv()

                @pl.when(has_right)
                def _():
                    piece(i, before, yy, True).start()

        @pl.when(z + t < n)
        def _():
            for yy in (y, oy):
                piece(i, after, yy, False).wait_recv()

                @pl.when(has_left)
                def _():
                    piece(i, after, yy, False).start()

    def all_sent(piece, i):
        @pl.loop(0, n)
        def _(t):
            before, after = ends(t)
            for yy in (y, oy):
                @pl.when(jnp.logical_and(z - t >= 0, has_right))
                def _():
                    piece(i, before, yy, True).wait_send()

                @pl.when(jnp.logical_and(z + t < n, has_left))
                def _():
                    piece(i, after, yy, False).wait_send()

    own_pieces(up_piece, 0, y)
    y_up = [send(up_peer.at[j], up_w.at[j, here], to_y) for j in range(tiles)]

    loads[2].wait()
    block = min(64, rows)

    @pl.loop(0, rows // block)
    def _(i):
        at = pl.ds(pl.multiple_of(i * block, block), block)
        wide = hid[at].astype(jnp.float32)
        scale = lax.rsqrt(jnp.mean(wide * wide, axis=1, keepdims=True) + 1e-06)
        tok[x, y, c, at] = (wide * scale * gain[...]).astype(LOW)

    loads[3].wait()
    for u in range(nsub):
        dn_w[z, u, y] = dn_st[0, :, u * pc:(u + 1) * pc].astype(LOW)
    loads[4].wait()
    for u in range(nsub):
        dn_peer[u] = dn_st[1, :, u * pc:(u + 1) * pc].astype(LOW)

    def token_part(xx, yy, first):
        return tok.at[xx, yy, c, pl.ds(0, top) if first else pl.ds(top, rows - top)]

    tx = [send(token_part(x, y, f), token_part(x, y, f), to_x) for f in (True, False)]
    ty = [send(token_part(x, y, f), token_part(x, y, f), to_y) for f in (False, True)]
    tc = send(tok.at[x, y, c], tok.at[x, y, c], to_c)

    def own_up(j):
        own_pieces(up_piece, j, y)

    def peer_up(j):
        y_up[j].wait_recv()
        own_pieces(up_piece, j, oy)

    def up_unit(gx, gy, j):
        at = pl.ds(pl.multiple_of(j * tile, tile), tile)
        sc_at = pl.ds(pl.multiple_of((x * 2 + y) * width + j * tile, tile), tile)
        pre = jnp.dot(
            tok[gx, gy].reshape(2 * rows, depth), up_w[j], preferred_element_type=jnp.float32
        )
        value = jnp.square(jnp.maximum(pre * up_scale[:, sc_at], 0.0)).astype(LOW)
        act[0, gx, gy, :, at] = value[:rows]
        act[1, gx, gy, :, at] = value[rows:]

    peer_up(0)
    if tiles > 1:
        own_up(1)
        peer_up(1)

    late = {}
    for j in range(tiles):
        last = j == tiles - 1
        if 2 <= j + 1 < tiles:
            own_up(j + 1)
            peer_up(j + 1)
        if last:
            own_pieces(dn_piece, 0, y)
        for t in range(1, n):
            pass_on(up_piece, j, t)
            if j == 0 and t == n - 1:
                tx[0].wait_recv()
                late["diag_y"] = send(token_part(ox, y, True), token_part(ox, y, True), to_y)
                late["y_dn"] = [send(dn_peer.at[u], dn_w.at[z, u, y], to_y) for u in range(nsub)]
            if j == tiles // 2 - 1 and t == n - 1:
                ty[0].wait_recv()
                late["diag_x"] = send(token_part(x, oy, False), token_part(x, oy, False), to_x)
                tx[1].wait_recv()
                cx = send(tok.at[ox, y, c], tok.at[ox, y, c], to_c)
            if j == tiles - 2:
                if t == max(1, n // 3):
                    tc.wait_recv()
                    cx.wait_recv()

                    @pl.loop(0, 2 * (tiles - 2))
                    def _(i):
                        g = i % 2
                        up_unit(x + g * (ox - x), y, i // 2)
                if t == max(1, (2 * n) // 3):
                    ty[1].wait_recv()
                    cy = send(tok.at[x, oy, c], tok.at[x, oy, c], to_c)
            if last:
                if t == 1:
                    cy.wait_recv()

                    @pl.loop(0, tiles - 1)
                    def _(i):
                        up_unit(x, oy, i)
                if t == max(1, n // 3):
                    late["diag_y"].wait_recv()
                    late["diag_x"].wait_recv()
                    cd = send(tok.at[ox, oy, c], tok.at[ox, oy, c], to_c)

                    @pl.loop(0, 2)
                    def _(g):
                        up_unit(x + g * (ox - x), y, tiles - 2)
                if t == max(1, (2 * n) // 3):
                    cd.wait_recv()

                    @pl.loop(0, tiles - 1)
                    def _(i):
                        up_unit(ox, oy, i)
    late["y_dn"][0].wait_recv()
    own_pieces(dn_piece, 0, oy)
    for u in range(1, nsub):
        own_pieces(dn_piece, u, y)
        late["y_dn"][u].wait_recv()
        own_pieces(dn_piece, u, oy)

    @pl.loop(0, 4)
    def _(i):
        up_unit(i // 2, i % 2, tiles - 1)

    side = jnp.minimum(z, n - 1 - z)
    far = jnp.where(z <= n - 1 - z, 1, -1)

    def owner(s):
        p = s // nsub
        near = z + (-1 if p % 2 else 1) * ((p + 1) // 2)
        return jnp.where(p <= 2 * side, near, z + far * (p - side))

    def each_part(s, cc, emit):
        o, u = owner(s), s % nsub

        @pl.loop(0, 2)
        def _(xx):
            left = act[cc, xx].reshape(2 * rows, width)
            if pc % 128 == 0:
                right = jnp.concatenate([dn_w[o, u, 0], dn_w[o, u, 1]], axis=1)
                both = jnp.dot(left, right, preferred_element_type=jnp.float32)
                halves = both[:, :pc], both[:, pc:]
            else:
                halves = [
                    jnp.dot(left, dn_w[o, u, yy], preferred_element_type=jnp.float32)
                    for yy in range(2)
                ]
            for yy in range(2):
                at = slice(yy * rows, (yy + 1) * rows)
                emit(0, xx, yy, halves[0][at].astype(LOW))
                emit(1, yy, xx, halves[1][at].astype(LOW))

    given, first, second = {}, {}, {}

    def for_partner(s):
        p = s % 2
        if s >= 2:
            given[s - 2].wait_send()

        def emit(h, f, g, part):
            psend[p, h, f, g] = part

        each_part(s, oc, emit)
        given[s] = send(psend.at[p], precv.at[s], to_c)

    slots = csum.shape[0]

    def for_own(s):
        p = s % slots

        def emit(h, f, g, part):
            csum[p, h, f, g] = part

        each_part(s, c, emit)
        given[s].wait_recv()
        total = csum[p].astype(jnp.float32) + precv[s].astype(jnp.float32)
        csum[p] = total.astype(LOW)
        first[s] = (
            send(csum.at[p, 0, ox], ra1.at[s], to_x),
            send(csum.at[p, 1, oy], rb1.at[s], to_y),
        )

    def second_stage(s):
        p = s % slots
        pair = []
        for h, f, g, got, dst, other in (
            (0, x, oy, ra1, ra2, to_y), (1, y, ox, rb1, rb2, to_x)
        ):
            first[s][h].wait_recv()
            total = csum[p, h, f, g].astype(jnp.float32) + got[s, g].astype(jnp.float32)
            csum[p, h, f, g] = total.astype(LOW)
            pair.append(send(csum.at[p, h, f, g], dst.at[s], other))
        second[s] = pair

    def finish(s):
        p = s % slots
        o, u = owner(s), s % nsub
        for h, f, g, one, two in ((0, x, y, ra1, ra2), (1, y, x, rb1, rb2)):
            second[s][h].wait_recv()
            total = csum[p, h, f, g].astype(jnp.float32) + one[s, g].astype(jnp.float32)
            total = total + two[s].astype(jnp.float32)
            slot = (o * 2 + h) * nsub + u
            if pc % 128 == 0:
                at = pl.ds(pl.multiple_of(slot * pc, pc), pc)
                out[:, at] = (total * dn_scale[:, at]).astype(out.dtype)
            else:
                out[slot] = (total * dn_scale[slot]).astype(out.dtype)
        for copy in (*first[s], *second[s]):
            copy.wait_send()

    for s in range(steps):
        for_partner(s)
        for_own(s)
        if 1 <= s < steps - 1:
            second_stage(s - 1)
        if s >= 2:
            finish(s - 2)
        if s == steps - 2:
            second_stage(s)
        e = s - nsub + 1
        if 0 <= e < (n - 1) * nsub:
            pass_on(dn_piece, e % nsub, e // nsub + 1)
    second_stage(steps - 1)
    finish(steps - 2)
    finish(steps - 1)
    for j in range(tiles):
        all_sent(up_piece, j)
    for u in range(nsub):
        all_sent(dn_piece, u)
    for copy in (
        *y_up, *tx, *ty, tc, late["diag_y"], *late["y_dn"], late["diag_x"], cx, cy, cd,
        given[steps - 2], given[steps - 1],
    ):
        copy.wait_send()


def body(hidden_in, norm_gain, up_weight, up_scale, down_weight, down_scale):
    n = lax.axis_size("fz")
    rows, depth = hidden_in.shape
    kr, cols = up_weight.shape[0], down_weight.shape[1]
    width = up_weight.shape[1] // 4
    tile = min(256, width)
    tiles = width // tile
    pc = min(128, cols)
    nsub = cols // pc
    steps = n * nsub
    flat = pc % 128 == 0
    sends = tiles + 10 + nsub + 5 * steps
    vmem = pl.BlockSpec(memory_space=pltpu.VMEM)
    hbm = pl.BlockSpec(memory_space=pl.ANY)
    dma = pltpu.SemaphoreType.DMA
    made = pl.pallas_call(
        functools.partial(kernel, n),
        out_shape=pltpu.VMEM((rows, depth), LOW) if flat else jax.ShapeDtypeStruct((2 * steps, rows, pc), LOW),
        in_specs=[hbm, vmem, hbm, vmem, hbm, vmem],
        out_specs=vmem,
        scratch_shapes=[
            pltpu.VMEM((rows, depth), LOW),
            pltpu.VMEM((2, kr, width), jnp.float32),
            pltpu.VMEM((2, width, cols), jnp.float32),
            pltpu.VMEM((tiles, kr, tile), LOW),
            pltpu.VMEM((nsub, width, pc), LOW),
            pltpu.VMEM((2, 2, 2, rows, depth), LOW),
            pltpu.VMEM((tiles, depth, tile), LOW),
            pltpu.VMEM((n, nsub, 2, width, pc), LOW),
            pltpu.VMEM((2, 2, 2, rows, width), LOW),
            pltpu.VMEM((2, 2, 2, 2, rows, pc), LOW),
            pltpu.VMEM((steps, 2, 2, 2, rows, pc), LOW),
            pltpu.VMEM((3, 2, 2, 2, rows, pc), LOW),
            pltpu.VMEM((steps, 2, rows, pc), LOW),
            pltpu.VMEM((steps, 2, rows, pc), LOW),
            pltpu.VMEM((steps, rows, pc), LOW),
            pltpu.VMEM((steps, rows, pc), LOW),
            dma((tiles, 2 * n)), dma((tiles, 2 * n)), dma((tiles, 2 * n)),
            dma((nsub, 2 * n)), dma((nsub, 2 * n)), dma((nsub, 2 * n)),
            dma((sends,)), dma((sends,)), dma((5,)),
        ],
        compiler_params=pltpu.CompilerParams(
            collective_id=0, has_side_effects=True, vmem_limit_bytes=(56000 if flat else 64000) * 1024
        ),
    )(
        hidden_in,
        norm_gain.reshape(1, depth),
        up_weight,
        up_scale.reshape(1, 4 * width),
        down_weight,
        down_scale.reshape((1, depth) if flat else (2 * steps, 1, pc)),
    )
    return made if flat else made.transpose(1, 0, 2).reshape(rows, depth)


def solution(mesh):
    n_rep, n_fs, n_tp = (mesh.shape[a] for a in ("rep", "fs", "tp"))
    split = Mesh(mesh.devices.reshape(n_rep, n_fs // 2, 2, n_tp), ("rep", "fz", "fy", "tp"))
    fs = ("fz", "fy")
    tokens = P(("rep", *fs, "tp"), None)
    placed = (tokens, P(), P(fs, "tp"), P("tp"), P("tp", fs), P())
    return jax.shard_map(body, mesh=split, in_specs=placed, out_specs=tokens, check_vma=False)
```

```python
import functools

import jax
import jax.numpy as jnp
from jax import lax
from jax.experimental import pallas as pl
from jax.experimental.pallas import tpu as pltpu
from jax.sharding import Mesh, PartitionSpec as P

MESH = pl.DeviceIdType.MESH
LOW = jnp.bfloat16


def kernel(
    n, hidden, gain_in, up_f32, up_scale_in, dn_f32, dn_scale_in, out,
    gain, up_scale, dn_scale, hid, up_st, dn_st, up_peer, dn_peer,
    tok, up_w, dn_w, act, psend, precv, csum, ra1, rb1, ra2, rb2,
    up_rs, up_sr, up_sl, dn_rs, dn_sr, dn_sl, ss, rs, ls,
):
    x, z, y, c = (lax.axis_index(a) for a in ("rep", "fz", "fy", "tp"))
    ox, oy, oc = 1 - x, 1 - y, 1 - c
    to_x, to_y, to_c = {"rep": ox}, {"fy": oy}, {"tp": oc}
    to_right = {"fz": jnp.minimum(z + 1, n - 1)}
    to_left = {"fz": jnp.maximum(z - 1, 0)}
    has_right, has_left = z < n - 1, z > 0
    tiles, kr, tile = up_peer.shape
    nsub, width, pc = dn_peer.shape
    rows, depth = hid.shape
    top = max(rows // 48, 1) * 16

    def quarter(yy):
        return pl.ds(pl.multiple_of((x * 2 + yy) * width, width), width)

    def up_load(yy, side, lo, hi, sem):
        start = (x * 2 + yy) * width + lo
        return pltpu.make_async_copy(
            up_f32.at[:, pl.ds(pl.multiple_of(start, tile), hi - lo)],
            up_st.at[side, :, pl.ds(lo, hi - lo)], sem,
        )

    loads = [
        up_load(y, 0, 0, tile, ls.at[0]),
        up_load(oy, 1, 0, tile, ls.at[1]),
        pltpu.make_async_copy(hidden, hid, ls.at[2]),
        up_load(y, 0, tile, width, ls.at[3]),
        up_load(oy, 1, tile, width, ls.at[4]),
        pltpu.make_async_copy(dn_f32.at[quarter(y)], dn_st.at[0], ls.at[5]),
        pltpu.make_async_copy(dn_f32.at[quarter(oy)], dn_st.at[1], ls.at[6]),
        pltpu.make_async_copy(gain_in, gain, ls.at[7]),
        pltpu.make_async_copy(up_scale_in.at[:, quarter(y)], up_scale, ls.at[8]),
        pltpu.make_async_copy(dn_scale_in, dn_scale, ls.at[9]),
    ]
    loads[0].start()
    barrier = pltpu.get_barrier_semaphore()
    for other in (to_x, to_y, to_c):
        pl.semaphore_signal(barrier, inc=1, device_id=other, device_id_type=MESH)

    @pl.when(has_right)
    def _():
        pl.semaphore_signal(barrier, inc=1, device_id=to_right, device_id_type=MESH)

    @pl.when(has_left)
    def _():
        pl.semaphore_signal(barrier, inc=1, device_id=to_left, device_id_type=MESH)

    for copy in loads[1:]:
        copy.start()
    here = pl.ds(pl.multiple_of((z * 2 + y) * kr, kr), kr)

    def low_up(side, tile_range):
        for j in tile_range:
            value = up_st[side, :, j * tile:(j + 1) * tile].astype(LOW)
            if side == 0:
                up_w[j, here] = value
            else:
                up_peer[j] = value

    loads[0].wait()
    low_up(0, range(1))
    loads[1].wait()
    low_up(1, range(1))
    pl.semaphore_wait(barrier, 3 + jnp.minimum(z, 1) + jnp.minimum(n - 1 - z, 1))

    count = [0]
    sent = []

    def remote(src, dst, send_sem, recv_sem, other):
        return pltpu.make_async_remote_copy(
            src_ref=src, dst_ref=dst, send_sem=send_sem, recv_sem=recv_sem,
            device_id=other, device_id_type=MESH,
        )

    def send(src, dst, other):
        i = count[0]
        count[0] += 1
        copy = remote(src, dst, ss.at[i], rs.at[i], other)
        copy.start()
        sent.append(copy)
        return copy

    def up_piece(j, o, yy, right):
        shard = o * 2 + yy
        ref = up_w.at[j, pl.ds(pl.multiple_of(shard * kr, kr), kr)]
        sems = up_sr if right else up_sl
        return remote(ref, ref, sems.at[j, shard], up_rs.at[j, shard], to_right if right else to_left)

    def dn_piece(u, o, yy, right):
        ref = dn_w.at[o, u, yy]
        sems = dn_sr if right else dn_sl
        return remote(
            ref, ref, sems.at[u, o * 2 + yy], dn_rs.at[u, o * 2 + yy], to_right if right else to_left
        )

    def own_pieces(piece, i, yy):
        @pl.when(has_right)
        def _():
            piece(i, z, yy, True).start()

        @pl.when(has_left)
        def _():
            piece(i, z, yy, False).start()

    def ends(t):
        return jnp.maximum(z - t, 0), jnp.minimum(z + t, n - 1)

    def pass_on(piece, i, t, shards):
        before, after = ends(t)

        @pl.when(z - t >= 0)
        def _():
            for yy in shards:
                piece(i, before, yy, True).wait_recv()

                @pl.when(has_right)
                def _():
                    piece(i, before, yy, True).start()

        @pl.when(z + t < n)
        def _():
            for yy in shards:
                piece(i, after, yy, False).wait_recv()

                @pl.when(has_left)
                def _():
                    piece(i, after, yy, False).start()

    def all_sent(piece, i):
        @pl.loop(0, n)
        def _(t):
            before, after = ends(t)
            for yy in (y, oy):
                @pl.when(jnp.logical_and(z - t >= 0, has_right))
                def _():
                    piece(i, before, yy, True).wait_send()

                @pl.when(jnp.logical_and(z + t < n, has_left))
                def _():
                    piece(i, after, yy, False).wait_send()

    def send_peer(j):
        return send(up_peer.at[j], up_w.at[j, here], to_y)

    own_pieces(up_piece, 0, y)
    y_up = [send_peer(0)]
    loads[3].wait()
    low_up(0, range(1, tiles))
    loads[4].wait()
    low_up(1, range(1, tiles))
    loads[2].wait()
    loads[7].wait()
    y_up += [send_peer(j) for j in range(1, tiles)]
    block = min(64, rows)

    @pl.loop(0, rows // block)
    def _(i):
        at = pl.ds(pl.multiple_of(i * block, block), block)
        wide = hid[at].astype(jnp.float32)
        scale = lax.rsqrt(jnp.mean(wide * wide, axis=1, keepdims=True) + 1e-06)
        tok[x, y, c, at] = (wide * scale * gain[...]).astype(LOW)

    loads[5].wait()
    for u in range(nsub):
        dn_w[z, u, y] = dn_st[0, :, u * pc:(u + 1) * pc].astype(LOW)
    loads[6].wait()
    for u in range(nsub):
        dn_peer[u] = dn_st[1, :, u * pc:(u + 1) * pc].astype(LOW)

    loads[8].wait()
    loads[9].wait()

    def token_part(xx, yy, first):
        return tok.at[xx, yy, c, pl.ds(0, top) if first else pl.ds(top, rows - top)]

    tx = [send(token_part(x, y, f), token_part(x, y, f), to_x) for f in (True, False)]
    ty = [send(token_part(x, y, f), token_part(x, y, f), to_y) for f in (False, True)]
    tc = send(tok.at[x, y, c], tok.at[x, y, c], to_c)

    def own_up(j):
        own_pieces(up_piece, j, y)

    def peer_up(j):
        y_up[j].wait_recv()
        own_pieces(up_piece, j, oy)

    def up_unit(gx, gy, j):
        at = pl.ds(pl.multiple_of(j * tile, tile), tile)
        pre = jnp.dot(
            tok[gx, gy].reshape(2 * rows, depth), up_w[j], preferred_element_type=jnp.float32
        )
        value = jnp.square(jnp.maximum(pre * up_scale[:, at], 0.0)).astype(LOW)
        act[0, gx, gy, :, at] = value[:rows]
        act[1, gx, gy, :, at] = value[rows:]

    peer_up(0)
    if tiles > 1:
        own_up(1)
        peer_up(1)

    late = {}
    for j in range(tiles):
        last = j == tiles - 1
        if 2 <= j + 1 < tiles:
            own_up(j + 1)
            peer_up(j + 1)
        if last:
            own_pieces(dn_piece, 0, y)
        for t in range(1, n):
            pass_on(up_piece, j, t, (y, oy))
            if j == 0 and t == n - 1:
                tx[0].wait_recv()
                late["diag_y"] = send(token_part(ox, y, True), token_part(ox, y, True), to_y)
                late["y_dn"] = [send(dn_peer.at[u], dn_w.at[z, u, y], to_y) for u in range(nsub)]
            if j == tiles // 2 - 1 and t == n - 1:
                ty[0].wait_recv()
                late["diag_x"] = send(token_part(x, oy, False), token_part(x, oy, False), to_x)
                tx[1].wait_recv()
                cx = send(tok.at[ox, y, c], tok.at[ox, y, c], to_c)
            if j == tiles - 2:
                if t == max(1, n // 3):
                    tc.wait_recv()
                    cx.wait_recv()

                    @pl.loop(0, 2 * (tiles - 2))
                    def _(i):
                        g = i % 2
                        up_unit(x + g * (ox - x), y, i // 2)
                if t == max(1, (2 * n) // 3):
                    ty[1].wait_recv()
                    cy = send(tok.at[x, oy, c], tok.at[x, oy, c], to_c)
            if last:
                if t == 1:
                    cy.wait_recv()

                    @pl.loop(0, tiles - 1)
                    def _(i):
                        up_unit(x, oy, i)
                if t == max(1, n // 3):
                    late["diag_y"].wait_recv()
                    late["diag_x"].wait_recv()
                    cd = send(tok.at[ox, oy, c], tok.at[ox, oy, c], to_c)

                    @pl.loop(0, 2)
                    def _(g):
                        up_unit(x + g * (ox - x), y, tiles - 2)
                if t == max(1, (2 * n) // 3):
                    cd.wait_recv()

                    @pl.loop(0, tiles - 1)
                    def _(i):
                        up_unit(ox, oy, i)
    late["y_dn"][0].wait_recv()
    own_pieces(dn_piece, 0, oy)
    for u in range(1, nsub):
        own_pieces(dn_piece, u, y)
        late["y_dn"][u].wait_recv()
        own_pieces(dn_piece, u, oy)

    @pl.loop(0, 4)
    def _(i):
        up_unit(i // 2, i % 2, tiles - 1)

    side = jnp.minimum(z, n - 1 - z)
    far = jnp.where(z <= n - 1 - z, 1, -1)
    half = rows // 2
    plan = [(p, u, None) for p in range(n) for u in range(nsub)]
    if pc % 128 == 0:
        plan = plan[:-1] + [(n - 1, nsub - 1, 0), (n - 1, nsub - 1, 1)]
    steps = len(plan)
    slots = csum.shape[0]

    def span(s):
        return pl.ds(0, rows if plan[s][2] is None else half)

    def owner(p):
        near = z + (-1 if p % 2 else 1) * ((p + 1) // 2)
        return jnp.where(p <= 2 * side, near, z + far * (p - side))

    def parts(s, cc, xx, dst):
        p, u, single = plan[s]
        o = owner(p)
        left = act[cc, xx].reshape(2 * rows, width)

        def dot(right):
            return jnp.dot(left, right, preferred_element_type=jnp.float32)

        if single is not None:
            one = dot(dn_w[o, u, single])
            for yy in range(2):
                for h in range(2):
                    at = yy * rows + h * half
                    dst[yy, h, pl.ds(0, half)] = one[at:at + half].astype(LOW)
            return
        if pc % 128 == 0:
            both = dot(jnp.concatenate([dn_w[o, u, 0], dn_w[o, u, 1]], axis=1))
            halves = both[:, :pc], both[:, pc:]
        else:
            halves = [dot(dn_w[o, u, yy]) for yy in range(2)]
        for yy in range(2):
            for h in range(2):
                dst[yy, h] = halves[h][yy * rows:(yy + 1) * rows].astype(LOW)

    given, first, second = {}, {}, {}

    def for_partner(s):
        p = s % 2
        if s >= 2:
            for copy in given[s - 2]:
                copy.wait_send()
        given[s] = []
        at = span(s)
        for i, xx in enumerate((ox, x)):
            parts(s, oc, xx, psend.at[p, i])
            given[s].append(
                send(psend.at[p, i, :, :, at], precv.at[s, i, :, :, at], to_c)
            )

    def for_own(s):
        p, at = s % slots, span(s)

        def first_send(i, yy, h, dst, k, other):
            return send(csum.at[p, i, yy, h, at], dst.at[s, k, at], other)

        for i, xx in enumerate((ox, x)):
            parts(s, c, xx, csum.at[p, i])
            given[s][i].wait_recv()
            mine, theirs = csum[p, i, :, :, at], precv[s, i, :, :, at]
            total = mine.astype(jnp.float32) + theirs.astype(jnp.float32)
            csum[p, i, :, :, at] = total.astype(LOW)
            if i == 0:
                first[s] = [
                    first_send(0, oy, 0, ra1, 0, to_x),
                    first_send(0, oy, 1, rb1, 0, to_y),
                    first_send(0, y, 0, ra1, 1, to_x),
                ]
        first[s].append(first_send(1, oy, 1, rb1, 1, to_y))

    def second_stage(s):
        p, at = s % slots, span(s)
        second[s] = []
        for h, i, yy, got, dst, other in ((0, 1, oy, ra1, ra2, to_y), (1, 0, y, rb1, rb2, to_x)):
            first[s][h].wait_recv()
            total = csum[p, i, yy, h, at].astype(jnp.float32) + got[s, 0, at].astype(jnp.float32)
            csum[p, i, yy, h, at] = total.astype(LOW)
            second[s].append(send(csum.at[p, i, yy, h, at], dst.at[s, at], other))

    def finish(s):
        q, at = s % slots, span(s)
        p, u, single = plan[s]
        for h, one, two in ((0, ra1, ra2), (1, rb1, rb2)):
            first[s][2 + h].wait_recv()
            second[s][h].wait_recv()
            total = csum[q, 1, y, h, at].astype(jnp.float32) + one[s, 1, at].astype(jnp.float32)
            total = total + two[s, at].astype(jnp.float32)
            slot = (owner(p) * 2 + (h if single is None else single)) * nsub + u
            put = pl.ds(0, rows) if single is None else pl.ds(h * half, half)
            if pc % 128 == 0:
                to = pl.ds(pl.multiple_of(slot * pc, pc), pc)
                out[put, to] = (total * dn_scale[:, to]).astype(out.dtype)
            else:
                out[slot, put] = (total * dn_scale[slot]).astype(out.dtype)
        for copy in (*first[s], *second[s]):
            copy.wait_send()

    events = [(t, u, (0, 1)) for t in range(1, n) for u in range(nsub)]
    if pc % 128 == 0:
        events = events[:-1] + [(n - 1, nsub - 1, (0,)), (n - 1, nsub - 1, (1,))]
    for s in range(steps):
        for_partner(s)
        for_own(s)
        if s >= 1 and s != steps - 2:
            second_stage(s - 1)
        if s >= 2:
            finish(s - 2)
        if s == steps - 3:
            second_stage(s)
        if s == 1:
            for j in range(tiles):
                all_sent(up_piece, j)
            for copy in (*y_up, *tx, *ty, tc, cx, cy, cd, *late["y_dn"]):
                copy.wait_send()
            late["diag_y"].wait_send()
            late["diag_x"].wait_send()
        e = s - nsub + 1
        if 0 <= e < len(events):
            t, u, shards = events[e]
            pass_on(dn_piece, u, t, shards)
    second_stage(steps - 1)
    finish(steps - 2)
    finish(steps - 1)
    for u in range(nsub):
        all_sent(dn_piece, u)
    for s in (steps - 2, steps - 1):
        for copy in given[s]:
            copy.wait_send()


def body(hidden_in, norm_gain, up_weight, up_scale, down_weight, down_scale):
    n = lax.axis_size("fz")
    rows, depth = hidden_in.shape
    kr, cols = up_weight.shape[0], down_weight.shape[1]
    width = up_weight.shape[1] // 4
    tile = min(256, width)
    tiles = width // tile
    pc = min(128, cols)
    nsub = cols // pc
    pieces = n * nsub
    flat = pc % 128 == 0
    steps = pieces + (1 if flat else 0)
    sends = tiles + 10 + nsub + 8 * steps
    vmem = pl.BlockSpec(memory_space=pltpu.VMEM)
    hbm = pl.BlockSpec(memory_space=pl.ANY)
    dma = pltpu.SemaphoreType.DMA
    made = pl.pallas_call(
        functools.partial(kernel, n),
        out_shape=pltpu.VMEM((rows, depth), LOW) if flat else jax.ShapeDtypeStruct((2 * pieces, rows, pc), LOW),
        in_specs=[hbm] * 6,
        out_specs=vmem,
        scratch_shapes=[
            pltpu.VMEM((1, depth), jnp.float32),
            pltpu.VMEM((1, width), jnp.float32),
            pltpu.VMEM((1, depth) if flat else (2 * pieces, 1, pc), jnp.float32),
            pltpu.VMEM((rows, depth), LOW),
            pltpu.VMEM((2, kr, width), jnp.float32),
            pltpu.VMEM((2, width, cols), jnp.float32),
            pltpu.VMEM((tiles, kr, tile), LOW),
            pltpu.VMEM((nsub, width, pc), LOW),
            pltpu.VMEM((2, 2, 2, rows, depth), LOW),
            pltpu.VMEM((tiles, depth, tile), LOW),
            pltpu.VMEM((n, nsub, 2, width, pc), LOW),
            pltpu.VMEM((2, 2, 2, rows, width), LOW),
            pltpu.VMEM((2, 2, 2, 2, rows, pc), LOW),
            pltpu.VMEM((steps, 2, 2, 2, rows, pc), LOW),
            pltpu.VMEM((3, 2, 2, 2, rows, pc), LOW),
            pltpu.VMEM((steps, 2, rows, pc), LOW),
            pltpu.VMEM((steps, 2, rows, pc), LOW),
            pltpu.VMEM((steps, rows, pc), LOW),
            pltpu.VMEM((steps, rows, pc), LOW),
            dma((tiles, 2 * n)), dma((tiles, 2 * n)), dma((tiles, 2 * n)),
            dma((nsub, 2 * n)), dma((nsub, 2 * n)), dma((nsub, 2 * n)),
            dma((sends,)), dma((sends,)), dma((10,)),
        ],
        compiler_params=pltpu.CompilerParams(
            collective_id=0, has_side_effects=True, vmem_limit_bytes=(57000 if flat else 65400) * 1024
        ),
    )(
        hidden_in,
        norm_gain.reshape(1, depth),
        up_weight,
        up_scale.reshape(1, 4 * width),
        down_weight,
        down_scale.reshape((1, depth) if flat else (2 * pieces, 1, pc)),
    )
    return made if flat else made.transpose(1, 0, 2).reshape(rows, depth)


def solution(mesh):
    n_rep, n_fs, n_tp = (mesh.shape[a] for a in ("rep", "fs", "tp"))
    split = Mesh(mesh.devices.reshape(n_rep, n_fs // 2, 2, n_tp), ("rep", "fz", "fy", "tp"))
    fs = ("fz", "fy")
    tokens = P(("rep", *fs, "tp"), None)
    placed = (tokens, P(), P(fs, "tp"), P("tp"), P("tp", fs), P())
    return jax.shard_map(body, mesh=split, in_specs=placed, out_specs=tokens, check_vma=False)
```
